32 devices in a mesh: rep: 2 (over x), fs: 8 (over z, y), tp: 2 (over core).
Axes of the slice: x: 2, y: 2, z: 4, core: 2. Of those that a mesh axis runs over, the one named last changes fastest.
Arguments:
- resid: bfloat16 [16384, 2048], P(('rep', 'fs'), 'tp'), may hold values from -6 to 6
- gain_mix_in: float32 [2048], replicated, may hold values from 0.1 to 1.9
- u_weight: float32 [2048, 1024], P('fs', 'tp'), may hold values from -0.125 to 0.125
- v_weight: float32 [2048, 1024], P('fs', 'tp'), may hold values from -0.125 to 0.125
- u_scale: float32 [1024], P('tp'), may hold values from 0.5 to 2
- v_scale: float32 [1024], P('tp'), may hold values from 0.3 to 3
- v_gain: float32 [1024], P('tp'), may hold values from 0.1 to 1.9
- mix_matrix: float32 [16, 128, 128], P('tp'), may hold values from -0.5 to 0.5
- mix_bias: float32 [16, 128], P('tp'), may hold values from 0.1 to 1.9
- out_weight: float32 [1024, 2048], P('tp', 'fs'), may hold values from -0.1875 to 0.1875
- out_scale: float32 [2048], P('fs'), may hold values from 0.3 to 3
- gain_mix_out: float32 [2048], replicated, may hold values from 0.1 to 1.9
- gain_ffn_in: float32 [2048], replicated, may hold values from 0.1 to 1.9
- up_weight: float32 [2048, 4096], P('fs', 'tp'), may hold values from -0.125 to 0.125
- up_scale: float32 [4096], P('tp'), may hold values from 0.5 to 2
- down_weight: float32 [4096, 2048], P('tp', 'fs'), may hold values from -0.09375 to 0.09375
- down_scale: float32 [2048], P('fs'), may hold values from 0.3 to 3
- gain_ffn_out: float32 [2048], replicated, may hold values from 0.1 to 1.9
Outputs:
- result: bfloat16 [16384, 2048], P(('rep', 'fs'), 'tp')
The draws below stay inside these ranges and needn't reach their ends.
All inputs are finite; a program needn't handle non-finite values.
Results may differ from the reference program's by a relative error of at most 0.013.
Values may be sent and summed in bfloat16 or wider, within the bound.
A program may use at most 128 MiB of HBM per device.

```python
import math
import jax
import jax.numpy as jnp
from jax import lax

D = 2048
A = 1024
GROUPS = 16
FF = 4096
BLOCK = 128
TOKENS = 16384
N_TP = 2


def shard_levels(key, dims, split, smallest, high):
    loudness = 1.0
    for dim, shards_of in split:
        heights = jax.random.uniform(jax.random.fold_in(jax.random.fold_in(key, 6), dim), (shards_of,), jnp.float32, smallest / len(split), high / len(split))
        loudness = loudness * jnp.repeat(jnp.exp(heights), dims[dim] // shards_of).reshape((-1,) + (1,) * (len(dims) - 1 - dim))
    return loudness


def normal_values(own_key, dims, scale, bound, shards=(), kind=jnp.bfloat16):
    loudness = shard_levels(own_key, dims, shards, -0.22, 0.18) if shards else 1.0
    drawn = jax.random.normal(own_key, dims, jnp.float32) * scale * loudness
    return jnp.minimum(jnp.maximum(drawn, -bound), bound).astype(kind)


def setup_inputs(seed: int = 0) -> dict:
    streams_of = jax.random.split(jax.random.key(seed), 19)
    return {
        "resid": normal_values(streams_of[0], (TOKENS, D), 1.0, 6.0, ((0, 16), (1, 2))),
        "gain_mix_in": jnp.clip(1.0 + 0.18 * jax.random.normal(streams_of[1], (D,), jnp.float32), 0.1, 1.9),
        "u_weight": normal_values(streams_of[2], (D, A), D ** -0.5, 0.125, ((0, 8), (1, 2)), jnp.float32),
        "v_weight": normal_values(streams_of[3], (D, A), D ** -0.5, 0.125, ((0, 8), (1, 2)), jnp.float32),
        "u_scale": jnp.clip(jnp.exp(math.log(2.0) - 1.3862944 * jax.random.uniform(streams_of[4], (A,), jnp.float32) ** shard_levels(streams_of[4], (A,), ((0, 2),), -0.2, 0.2)), 0.5, 2.0),
        "v_scale": jnp.clip(jnp.exp(math.log(3.0) - 2.3025851 * jax.random.uniform(streams_of[5], (A,), jnp.float32) ** shard_levels(streams_of[5], (A,), ((0, 2),), -0.2, 0.2)), 0.3, 3.0),
        "v_gain": jnp.clip(1.0 + 0.18 * jax.random.normal(streams_of[6], (A,), jnp.float32), 0.1, 1.9),
        "mix_matrix": normal_values(streams_of[7], (GROUPS, BLOCK, BLOCK), BLOCK ** -0.5, 0.5, ((0, 2),), jnp.float32),
        "mix_bias": jnp.clip(1.0 + 0.18 * jax.random.normal(streams_of[8], (GROUPS, BLOCK), jnp.float32), 0.1, 1.9),
        "out_weight": normal_values(streams_of[9], (A, D), A ** -0.5, 0.1875, ((0, 2), (1, 8)), jnp.float32),
        "out_scale": jnp.clip(jnp.exp(math.log(3.0) - 2.3025851 * jax.random.uniform(streams_of[10], (D,), jnp.float32) ** shard_levels(streams_of[10], (D,), ((0, 8),), -0.2, 0.2)), 0.3, 3.0),
        "gain_mix_out": jnp.clip(1.0 + 0.18 * jax.random.normal(streams_of[11], (D,), jnp.float32), 0.1, 1.9),
        "gain_ffn_in": jnp.clip(1.0 + 0.18 * jax.random.normal(streams_of[12], (D,), jnp.float32), 0.1, 1.9),
        "up_weight": normal_values(streams_of[13], (D, FF), D ** -0.5, 0.125, ((0, 8), (1, 2)), jnp.float32),
        "up_scale": jnp.clip(jnp.exp(math.log(2.0) - 1.3862944 * jax.random.uniform(streams_of[14], (FF,), jnp.float32) ** shard_levels(streams_of[14], (FF,), ((0, 2),), -0.2, 0.2)), 0.5, 2.0),
        "down_weight": normal_values(streams_of[15], (FF, D), FF ** -0.5, 0.09375, ((0, 2), (1, 8)), jnp.float32),
        "down_scale": jnp.clip(jnp.exp(math.log(3.0) - 2.3025851 * jax.random.uniform(streams_of[16], (D,), jnp.float32) ** shard_levels(streams_of[16], (D,), ((0, 8),), -0.2, 0.2)), 0.3, 3.0),
        "gain_ffn_out": jnp.clip(1.0 + 0.18 * jax.random.normal(streams_of[17], (D,), jnp.float32), 0.1, 1.9),
    }


def rms_norm(values, gain):
    power = lax.optimization_barrier(jnp.mean(values * values, axis=-1, keepdims=True))
    return values * lax.rsqrt(power + 1e-06) * gain

def split_sum(left, right, pieces):
    width = left.shape[1] // pieces
    total = jnp.zeros((left.shape[0], right.shape[1]), jnp.float32)
    for index in range(pieces):
        lower = index * width
        partial_value = jnp.dot(left[:, lower:lower + width], right[lower:lower + width], preferred_element_type=jnp.float32)
        rounded = lax.optimization_barrier(partial_value.astype(jnp.bfloat16))
        total = total + rounded.astype(jnp.float32)
    return total

def reference(resid, gain_mix_in, u_weight, v_weight, u_scale, v_scale, v_gain, mix_matrix, mix_bias, out_weight, out_scale, gain_mix_out, gain_ffn_in, up_weight, up_scale, down_weight, down_scale, gain_ffn_out):
    stream = resid.astype(jnp.float32)
    normed = rms_norm(stream, gain_mix_in).astype(jnp.bfloat16)
    u_act = jax.nn.gelu(jnp.dot(normed, u_weight.astype(jnp.bfloat16), preferred_element_type=jnp.float32) * u_scale)
    v_act = jax.nn.gelu(jnp.dot(normed, v_weight.astype(jnp.bfloat16), preferred_element_type=jnp.float32) * v_scale)
    centre = lax.optimization_barrier(jnp.mean(v_act, axis=-1, keepdims=True))
    spread = lax.optimization_barrier(jnp.mean(jnp.square(v_act - centre), axis=-1, keepdims=True))
    v_norm = ((v_act - centre) * lax.rsqrt(spread + 1e-06) * v_gain).astype(jnp.bfloat16)
    tokens = resid.shape[0]
    groups = mix_matrix.shape[0]
    blocks = v_norm.reshape(tokens // BLOCK, BLOCK, groups, A // groups).astype(jnp.float32)
    matrix = mix_matrix.astype(jnp.bfloat16).astype(jnp.float32)
    mixed = jnp.einsum('gts,bsgd->btgd', matrix, blocks) + mix_bias.T[None, :, :, None]
    gated = (u_act * mixed.reshape(tokens, A)).astype(jnp.bfloat16)
    mix_out = split_sum(gated, out_weight.astype(jnp.bfloat16), N_TP) * out_scale
    middle = (stream + rms_norm(mix_out, gain_mix_out)).astype(jnp.bfloat16)
    ffn_in = rms_norm(middle.astype(jnp.float32), gain_ffn_in).astype(jnp.bfloat16)
    raised = jnp.dot(ffn_in, up_weight.astype(jnp.bfloat16), preferred_element_type=jnp.float32) * up_scale
    hidden = jnp.square(jax.nn.relu(raised)).astype(jnp.bfloat16)
    ffn_out = split_sum(hidden, down_weight.astype(jnp.bfloat16), N_TP) * down_scale
    return (middle.astype(jnp.float32) + rms_norm(ffn_out, gain_ffn_out)).astype(jnp.bfloat16)
```

```python
import functools

import jax
import jax.numpy as jnp
from jax import lax
from jax.experimental import pallas as pl
from jax.experimental.pallas import tpu as pltpu
from jax.sharding import PartitionSpec as P


def gather_kernel(by_rows, n_out, n_in, *refs):
    count = len(by_rows)
    srcs, resid = refs[:count], refs[count]
    dsts, other = refs[count + 1 : 2 * count + 1], refs[2 * count + 1]
    z_send, z_recv, y_send, y_recv, x_send, x_recv, t_send, t_recv, own_sem = refs[2 * count + 2 :]
    member = lax.axis_index("fs")
    rep = lax.axis_index("rep")
    tp = lax.axis_index("tp")
    outer, inner = member // n_in, member % n_in
    peer_in = 1 - inner

    def at(index):
        return {"fs": index}

    barrier = pltpu.get_barrier_semaphore()
    greeted = [at(lax.rem(outer + k, n_out) * n_in + inner) for k in range(1, n_out)]
    greeted += [at(outer * n_in + peer_in), {"rep": 1 - rep}, {"tp": 1 - tp}]
    for device in greeted:
        pl.semaphore_signal(barrier, inc=1, device_id=device, device_id_type=pl.DeviceIdType.MESH)
    pl.semaphore_wait(barrier, len(greeted))

    def slot(w, index, half=None):
        rows, cols = srcs[w].shape
        base, size = (0, rows) if half is None else (half * (rows // 2), rows // 2)
        if by_rows[w]:
            return dsts[w].at[pl.ds(pl.multiple_of(index * rows + base, 8), size), :]
        return dsts[w].at[pl.ds(base, size), pl.ds(pl.multiple_of(index * cols, 128), cols)]

    def remote(src, dst, send, recv, device):
        return pltpu.make_async_remote_copy(
            src_ref=src,
            dst_ref=dst,
            send_sem=send,
            recv_sem=recv,
            device_id=device,
            device_id_type=pl.DeviceIdType.MESH,
        )

    swap = remote(resid, other, t_send, t_recv, {"tp": 1 - tp})
    swap.start()
    own, z_copies, y_copies, x_copies = [], {}, {}, {}
    for w in range(count):
        for k in range(1, n_out):
            target = lax.rem(outer - k + n_out, n_out) * n_in + inner
            copy = remote(srcs[w], slot(w, member), z_send.at[w, k - 1], z_recv.at[w, k - 1], at(target))
            copy.start()
            z_copies[w, k] = copy
        local_copy = pltpu.make_async_copy(srcs[w], slot(w, member), own_sem.at[w])
        local_copy.start()
        own.append(local_copy)

    def cross_inner(w, k):
        index = lax.rem(outer + k, n_out) * n_in + inner
        rows = srcs[w].shape[0]
        if k:
            z_copies[w, k].wait_recv()
            source = slot(w, index, rep)
        else:
            source = srcs[w].at[pl.ds(pl.multiple_of(rep * (rows // 2), 8), rows // 2), :]
        copy = remote(source, slot(w, index, rep), y_send.at[w, k], y_recv.at[w, k], at(outer * n_in + peer_in))
        copy.start()
        y_copies[w, k] = copy

    def cross_rep(w, k):
        index = lax.rem(outer + k, n_out) * n_in + peer_in
        y_copies[w, k].wait_recv()
        landed = slot(w, index, rep)
        copy = remote(landed, landed, x_send.at[w, k], x_recv.at[w, k], {"rep": 1 - rep})
        copy.start()
        x_copies[w, k] = copy

    order = [(w, k) for w in range(count) for k in range(n_out)]
    lag = 2
    for step in range(len(order) + lag):
        if step < len(order):
            cross_inner(*order[step])
        if step >= lag:
            cross_rep(*order[step - lag])
    for item in order:
        x_copies[item].wait()
        y_copies[item].wait_send()
    for copy in z_copies.values():
        copy.wait_send()
    for copy in own:
        copy.wait()
    swap.wait()


def gather_all(shards, by_rows, resid):
    members = lax.axis_size("fs")
    n_in = 2
    n_out = members // n_in
    count = len(shards)
    shapes = []
    for shard, rowwise in zip(shards, by_rows):
        rows, cols = shard.shape
        full = (rows * members, cols) if rowwise else (rows, cols * members)
        shapes.append(jax.ShapeDtypeStruct(full, shard.dtype))
    shapes.append(jax.ShapeDtypeStruct(resid.shape, resid.dtype))
    pairs = [(count, n_out - 1)] * 2 + [(count, n_out)] * 4
    return pl.pallas_call(
        functools.partial(gather_kernel, by_rows, n_out, n_in),
        out_shape=shapes,
        in_specs=[pl.BlockSpec(memory_space=pltpu.VMEM)] * (count + 1),
        out_specs=[pl.BlockSpec(memory_space=pl.ANY)] * (count + 1),
        scratch_shapes=[pltpu.SemaphoreType.DMA(pair) for pair in pairs]
        + [pltpu.SemaphoreType.DMA, pltpu.SemaphoreType.DMA, pltpu.SemaphoreType.DMA((count,))],
        compiler_params=pltpu.CompilerParams(
            collective_id=0, has_side_effects=True, vmem_limit_bytes=32 * 1024 * 1024
        ),
    )(*shards, resid)


def rms_norm(values, gain, width, power_sum):
    return values * lax.rsqrt(power_sum / width + 1e-06) * gain


def local(
    resid,
    gain_mix_in,
    u_weight,
    v_weight,
    u_scale,
    v_scale,
    v_gain,
    mix_matrix,
    mix_bias,
    out_weight,
    out_scale,
    gain_mix_out,
    gain_ffn_in,
    up_weight,
    up_scale,
    down_weight,
    down_scale,
    gain_ffn_out,
):
    rows = resid.shape[0]
    part_width = resid.shape[1]
    width = part_width * lax.axis_size("tp")
    lane = lax.axis_index("tp")
    full_rows = lax.all_gather(resid, "tp", axis=1, tiled=True)
    out_scales, down_scales = (
        lax.all_gather(out_scale, "fs", axis=0, tiled=True),
        lax.all_gather(down_scale, "fs", axis=0, tiled=True),
    )
    full_float = full_rows.astype(jnp.float32)
    normed = rms_norm(
        full_float, gain_mix_in, width, jnp.sum(full_float * full_float, axis=1, keepdims=True)
    ).astype(jnp.bfloat16)
    branch_cols = u_weight.shape[1]
    u_pre = jnp.dot(
        normed,
        lax.all_gather(u_weight.astype(jnp.bfloat16), "fs", axis=0, tiled=True),
        preferred_element_type=jnp.float32,
    )
    v_pre = jnp.dot(
        normed,
        lax.all_gather(v_weight.astype(jnp.bfloat16), "fs", axis=0, tiled=True),
        preferred_element_type=jnp.float32,
    )
    u_act = jax.nn.gelu(u_pre * u_scale)
    v_act = jax.nn.gelu(v_pre * v_scale)
    total, squares = lax.psum(
        (jnp.sum(v_act, axis=1, keepdims=True), jnp.sum(v_act * v_act, axis=1, keepdims=True)), "tp"
    )
    branch_width = branch_cols * lax.axis_size("tp")
    centre = total / branch_width
    spread = squares / branch_width - centre * centre
    v_norm = ((v_act - centre) * lax.rsqrt(spread + 1e-06) * v_gain).astype(jnp.bfloat16)
    groups = mix_matrix.shape[0]
    block = mix_matrix.shape[1]
    blocks = v_norm.reshape(rows // block, block, groups, branch_cols // groups)
    mixed = (
        jnp.einsum(
            "gts,bsgd->btgd",
            mix_matrix.astype(jnp.bfloat16),
            blocks,
            preferred_element_type=jnp.float32,
        )
        + mix_bias.T[None, :, :, None]
    )
    gated = (u_act * mixed.reshape(rows, branch_cols)).astype(jnp.bfloat16)
    partial_value = jnp.dot(
        gated,
        lax.all_gather(out_weight.astype(jnp.bfloat16), "fs", axis=1, tiled=True),
        preferred_element_type=jnp.float32,
    )
    mix_out = lax.psum(partial_value.astype(jnp.bfloat16), "tp").astype(jnp.float32) * out_scales
    power = jnp.sum(mix_out * mix_out, axis=1, keepdims=True)
    middle_full = (full_float + rms_norm(mix_out, gain_mix_out, width, power)).astype(jnp.bfloat16)
    middle = lax.dynamic_slice_in_dim(middle_full, lane * part_width, part_width, 1)
    middle_float = middle_full.astype(jnp.float32)
    ffn_in = rms_norm(
        middle_float,
        gain_ffn_in,
        width,
        jnp.sum(middle_float * middle_float, axis=1, keepdims=True),
    ).astype(jnp.bfloat16)
    up_half = up_weight.astype(jnp.bfloat16)
    down_half = down_weight.astype(jnp.bfloat16)
    whole_up = lax.all_gather(up_half, "fs", axis=0, tiled=True)
    raised = jnp.dot(ffn_in, whole_up, preferred_element_type=jnp.float32)
    hidden = jnp.square(jax.nn.relu(raised * up_scale)).astype(jnp.bfloat16)
    whole_down = lax.all_gather(down_half, "fs", axis=1, tiled=True)
    terms = jnp.dot(hidden, whole_down, preferred_element_type=jnp.float32)
    own_down = lax.dynamic_slice_in_dim(down_scales, lane * part_width, part_width, 0)
    ffn_out = (
        lax.psum_scatter(terms.astype(jnp.bfloat16), "tp", scatter_dimension=1, tiled=True).astype(
            jnp.float32
        )
        * own_down
    )
    power_out = lax.psum(jnp.sum(ffn_out * ffn_out, axis=1, keepdims=True), "tp")
    own_gain_out = lax.dynamic_slice_in_dim(gain_ffn_out, lane * part_width, part_width, 0)
    return (middle.astype(jnp.float32) + rms_norm(ffn_out, own_gain_out, width, power_out)).astype(
        jnp.bfloat16
    )


def local_fast(
    resid,
    gain_mix_in,
    u_weight,
    v_weight,
    u_scale,
    v_scale,
    v_gain,
    mix_matrix,
    mix_bias,
    out_weight,
    out_scale,
    gain_mix_out,
    gain_ffn_in,
    up_weight,
    up_scale,
    down_weight,
    down_scale,
    gain_ffn_out,
):
    rows = resid.shape[0]
    part_width = resid.shape[1]
    width = part_width * lax.axis_size("tp")
    lane = lax.axis_index("tp")
    half = jnp.bfloat16
    scale_cols = out_scale.shape[0]
    scales = jnp.concatenate(
        [jnp.broadcast_to(out_scale, (8, scale_cols)), jnp.broadcast_to(down_scale, (8, scale_cols))]
    )
    shards = [
        v_weight.astype(half),
        u_weight.astype(half),
        out_weight.astype(half),
        scales,
        up_weight.astype(half),
        down_weight.astype(half),
    ]
    whole_v, whole_u, whole_out, whole_scales, whole_up, whole_down, other = gather_all(
        shards, (True, True, False, True, True, False), resid
    )
    whole_scales = whole_scales.reshape(-1, 16, scale_cols)
    out_scales, down_scales = whole_scales[:, 0].reshape(-1), whole_scales[:, 8].reshape(-1)
    swap = [(0, 1), (1, 0)]
    full_rows = jnp.where(
        lane == 0,
        jnp.concatenate([resid, other], axis=1),
        jnp.concatenate([other, resid], axis=1),
    )
    full_float = full_rows.astype(jnp.float32)
    normed = rms_norm(
        full_float, gain_mix_in, width, jnp.sum(full_float * full_float, axis=1, keepdims=True)
    ).astype(jnp.bfloat16)
    branch_cols = u_weight.shape[1]
    u_pre = jnp.dot(
        normed,
        whole_u,
        preferred_element_type=jnp.float32,
    )
    v_pre = jnp.dot(
        normed,
        whole_v,
        preferred_element_type=jnp.float32,
    )
    u_act = jax.nn.gelu(u_pre * u_scale)
    v_act = jax.nn.gelu(v_pre * v_scale)
    total, squares = lax.psum(
        (jnp.sum(v_act, axis=1, keepdims=True), jnp.sum(v_act * v_act, axis=1, keepdims=True)), "tp"
    )
    branch_width = branch_cols * lax.axis_size("tp")
    centre = total / branch_width
    spread = squares / branch_width - centre * centre
    v_norm = ((v_act - centre) * lax.rsqrt(spread + 1e-06) * v_gain).astype(jnp.bfloat16)
    groups = mix_matrix.shape[0]
    block = mix_matrix.shape[1]
    blocks = v_norm.reshape(rows // block, block, groups, branch_cols // groups)
    mixed = (
        jnp.einsum(
            "gts,bsgd->btgd",
            mix_matrix.astype(jnp.bfloat16),
            blocks,
            preferred_element_type=jnp.float32,
        )
        + mix_bias.T[None, :, :, None]
    )
    gated = (u_act * mixed.reshape(rows, branch_cols)).astype(jnp.bfloat16)
    partial_value = jnp.dot(
        gated,
        whole_out,
        preferred_element_type=jnp.float32,
    )
    rounded = partial_value.astype(half)
    mix_out = (
        rounded.astype(jnp.float32) + lax.ppermute(rounded, "tp", swap).astype(jnp.float32)
    ) * out_scales
    power = jnp.sum(mix_out * mix_out, axis=1, keepdims=True)
    middle_full = (full_float + rms_norm(mix_out, gain_mix_out, width, power)).astype(jnp.bfloat16)
    middle = lax.dynamic_slice_in_dim(middle_full, lane * part_width, part_width, 1)
    middle_float = middle_full.astype(jnp.float32)
    ffn_in = rms_norm(
        middle_float,
        gain_ffn_in,
        width,
        jnp.sum(middle_float * middle_float, axis=1, keepdims=True),
    ).astype(jnp.bfloat16)
    raised = jnp.dot(ffn_in, whole_up, preferred_element_type=jnp.float32)
    hidden = jnp.square(jax.nn.relu(raised * up_scale)).astype(jnp.bfloat16)
    terms = jnp.dot(hidden, whole_down, preferred_element_type=jnp.float32)
    own_down = lax.dynamic_slice_in_dim(down_scales, lane * part_width, part_width, 0)
    terms = terms.astype(half)
    kept = lax.dynamic_slice_in_dim(terms, lane * part_width, part_width, 1)
    sent = lax.dynamic_slice_in_dim(terms, (1 - lane) * part_width, part_width, 1)
    ffn_out = (
        kept.astype(jnp.float32) + lax.ppermute(sent, "tp", swap).astype(jnp.float32)
    ) * own_down
    power_out = lax.psum(jnp.sum(ffn_out * ffn_out, axis=1, keepdims=True), "tp")
    own_gain_out = lax.dynamic_slice_in_dim(gain_ffn_out, lane * part_width, part_width, 0)
    return (middle.astype(jnp.float32) + rms_norm(ffn_out, own_gain_out, width, power_out)).astype(
        jnp.bfloat16
    )


def solution(mesh):
    in_specs = (
        P(("rep", "fs"), "tp"),
        P(),
        P("fs", "tp"),
        P("fs", "tp"),
        P("tp"),
        P("tp"),
        P("tp"),
        P("tp", None, None),
        P("tp", None),
        P("tp", "fs"),
        P("fs"),
        P(),
        P(),
        P("fs", "tp"),
        P("tp"),
        P("tp", "fs"),
        P("fs"),
        P(),
    )
    out_specs = P(("rep", "fs"), "tp")
    sizes = mesh.shape

    def whole(*args):
        columns = args[9].shape[1] // sizes["fs"]
        depth = args[2].shape[0] // sizes["fs"]
        paired = sizes["rep"] == 2 and sizes["tp"] == 2 and sizes["fs"] % 2 == 0
        fast = paired and columns % 128 == 0 and depth % 32 == 0
        return mapped(local_fast if fast else local)(*args)

    def mapped(body):
        return jax.shard_map(
            body, mesh=mesh, in_specs=in_specs, out_specs=out_specs, check_vma=False
        )

    return whole
```

```python
import functools

import jax
import jax.numpy as jnp
from jax import lax
from jax.experimental import pallas as pl
from jax.experimental.pallas import tpu as pltpu
from jax.sharding import PartitionSpec as P


def gather_kernel(by_rows, parts, n_out, n_in, *refs):
    count = len(by_rows)
    srcs, resid = refs[:count], refs[count]
    dsts, other = refs[count + 1 : 2 * count + 1], refs[2 * count + 1]
    z_send, z_recv, y_send, y_recv, x_send, x_recv, t_send, t_recv, own_sem = refs[2 * count + 2 :]
    member = lax.axis_index("fs")
    rep = lax.axis_index("rep")
    tp = lax.axis_index("tp")
    outer, inner = member // n_in, member % n_in
    peer_in = 1 - inner
    has_left, has_right = outer > 0, outer < n_out - 1
    left, right = {"fs": member - n_in}, {"fs": member + n_in}
    across, twin, mate = {"fs": outer * n_in + peer_in}, {"rep": 1 - rep}, {"tp": 1 - tp}

    def greet(device):
        pl.semaphore_signal(barrier, inc=1, device_id=device, device_id_type=pl.DeviceIdType.MESH)

    barrier = pltpu.get_barrier_semaphore()
    for step in (1, n_out - 1):
        greet({"fs": lax.rem(outer + step, n_out) * n_in + inner})
    for device in (across, twin, mate):
        greet(device)
    pl.semaphore_wait(barrier, 5)

    def slot(part, index, first=0, length=4):
        w, low, size = parts[part]
        rows, cols = srcs[w].shape
        base, size = low + first * (size // 4), length * (size // 4)
        if by_rows[w]:
            return dsts[w].at[pl.ds(pl.multiple_of(index * rows + base, 8), size), :]
        return dsts[w].at[
            pl.ds(pl.multiple_of(base, 8), size), pl.ds(pl.multiple_of(index * cols, 128), cols)
        ]

    def remote(ref, send, recv, device):
        return pltpu.make_async_remote_copy(
            src_ref=ref,
            dst_ref=ref,
            send_sem=send,
            recv_sem=recv,
            device_id=device,
            device_id_type=pl.DeviceIdType.MESH,
        )

    swap = pltpu.make_async_remote_copy(
        src_ref=resid,
        dst_ref=other,
        send_sem=t_send,
        recv_sem=t_recv,
        device_id=mate,
        device_id_type=pl.DeviceIdType.MESH,
    )
    own = []
    for w in range(count):
        rows, cols = srcs[w].shape
        if by_rows[w]:
            place = dsts[w].at[pl.ds(pl.multiple_of(member * rows, 8), rows), :]
        else:
            place = dsts[w].at[:, pl.ds(pl.multiple_of(member * cols, 128), cols)]
        own.append(pltpu.make_async_copy(srcs[w], place, own_sem.at[w]))
        own[w].start()

    def column(index, line):
        return index * n_in + line

    def z_copy(part, way, d, piece):
        ahead = 1 if way == 0 else -1
        index = column(outer - ahead * d, inner)
        ref = slot(part, index, 2 * rep, 2) if piece == 0 else slot(part, index, 3 * (1 - rep), 1)
        return remote(
            ref,
            z_send.at[part, way, d, piece],
            z_recv.at[part, way, d, piece],
            right if way == 0 else left,
        )

    def valid(way, d):
        return outer >= d if way == 0 else outer + d <= n_out - 1

    def onward(way):
        return has_right if way == 0 else has_left

    def source_of(way, d):
        return outer - d if way == 0 else outer + d

    def y_copy(part, way, d):
        ref = slot(part, column(source_of(way, d), inner), 2 * rep, 2)
        return remote(ref, y_send.at[part, way, d], y_recv.at[part, way, d], across)

    def y_own(part):
        ref = slot(part, member)
        return remote(ref, y_send.at[part, 0, 0], y_recv.at[part, 0, 0], across)

    def x_copy(part, way, d, piece):
        if piece == 0:
            ref = slot(part, column(source_of(way, d), inner), 1 + rep, 1)
        else:
            ref = slot(part, column(source_of(way, d), peer_in), 2 * rep, 2)
        return remote(ref, x_send.at[part, way, d, piece], x_recv.at[part, way, d, piece], twin)

    def landed(part, way, d, piece):
        index = column(source_of(way, d), inner)
        ref = slot(part, index, 2 * rep, 2) if piece == 0 else slot(part, index, 3 * (1 - rep), 1)
        remote(
            ref,
            z_send.at[part, way, d - 1, piece],
            z_recv.at[part, way, d - 1, piece],
            left if way == 0 else right,
        ).wait_recv()

    for w in range(count):
        own[w].wait()
        for part, (held, _, _) in enumerate(parts):
            if held == w:
                for way in range(2):

                    @pl.when(onward(way))
                    def _():
                        z_copy(part, way, 0, 0).start()
                        z_copy(part, way, 0, 1).start()

                y_own(part).start()
        if w == 0:
            swap.start()

    def first_stage(part, way, d):
        @pl.when(valid(way, d))
        def _():
            for piece in range(2):
                landed(part, way, d, piece)
                if d < n_out - 1:
                    pl.when(onward(way))(lambda: z_copy(part, way, d, piece).start())
                if piece == 0:
                    y_copy(part, way, d).start()
                    x_copy(part, way, d, 0).start()

    def second_stage(part, way, d):
        @pl.when(valid(way, d))
        def _():
            y_copy(part, way, d).wait_recv()
            x_copy(part, way, d, 1).start()

    order = [
        (part, way, d) for part in range(len(parts)) for d in range(1, n_out) for way in range(2)
    ]
    lag = 4
    for step in range(len(order) + lag):
        if step < len(order):
            first_stage(*order[step])
        if step >= lag:
            second_stage(*order[step - lag])
    for part, way, d in order:

        @pl.when(valid(way, d))
        def _():
            for piece in range(2):
                x_copy(part, way, d, piece).wait()
                if d < n_out - 1:
                    pl.when(onward(way))(lambda: z_copy(part, way, d, piece).wait_send())
            y_copy(part, way, d).wait_send()

    for part in range(len(parts)):
        y_own(part).wait()
        for way in range(2):

            @pl.when(onward(way))
            def _():
                z_copy(part, way, 0, 0).wait_send()
                z_copy(part, way, 0, 1).wait_send()

    swap.wait()


def gather_all(shards, by_rows, resid):
    members = lax.axis_size("fs")
    n_in = 2
    n_out = members // n_in
    count = len(shards)
    shapes = []
    for shard, rowwise in zip(shards, by_rows):
        rows, cols = shard.shape
        full = (rows * members, cols) if rowwise else (rows, cols * members)
        shapes.append(jax.ShapeDtypeStruct(full, shard.dtype))
    shapes.append(jax.ShapeDtypeStruct(resid.shape, resid.dtype))
    parts = []
    for w, shard in enumerate(shards):
        rows = shard.shape[0]
        pieces = 2 if w >= 4 else 1
        parts += [(w, piece * (rows // pieces), rows // pieces) for piece in range(pieces)]
    many = len(parts)
    pairs = [(many, 2, n_out, 2)] * 2 + [(many, 2, n_out)] * 2 + [(many, 2, n_out, 2)] * 2
    return pl.pallas_call(
        functools.partial(gather_kernel, by_rows, tuple(parts), n_out, n_in),
        out_shape=shapes,
        in_specs=[pl.BlockSpec(memory_space=pltpu.VMEM)] * (count + 1),
        out_specs=[pl.BlockSpec(memory_space=pl.ANY)] * (count + 1),
        scratch_shapes=[pltpu.SemaphoreType.DMA(pair) for pair in pairs]
        + [pltpu.SemaphoreType.DMA, pltpu.SemaphoreType.DMA, pltpu.SemaphoreType.DMA((count,))],
        compiler_params=pltpu.CompilerParams(
            collective_id=0, has_side_effects=True, vmem_limit_bytes=32 * 1024 * 1024
        ),
    )(*shards, resid)


def rms_norm(values, gain, width, power_sum):
    return values * lax.rsqrt(power_sum / width + 1e-06) * gain


def local(
    resid,
    gain_mix_in,
    u_weight,
    v_weight,
    u_scale,
    v_scale,
    v_gain,
    mix_matrix,
    mix_bias,
    out_weight,
    out_scale,
    gain_mix_out,
    gain_ffn_in,
    up_weight,
    up_scale,
    down_weight,
    down_scale,
    gain_ffn_out,
):
    rows = resid.shape[0]
    part_width = resid.shape[1]
    width = part_width * lax.axis_size("tp")
    lane = lax.axis_index("tp")
    full_rows = lax.all_gather(resid, "tp", axis=1, tiled=True)
    out_scales, down_scales = (
        lax.all_gather(out_scale, "fs", axis=0, tiled=True),
        lax.all_gather(down_scale, "fs", axis=0, tiled=True),
    )
    full_float = full_rows.astype(jnp.float32)
    normed = rms_norm(
        full_float, gain_mix_in, width, jnp.sum(full_float * full_float, axis=1, keepdims=True)
    ).astype(jnp.bfloat16)
    branch_cols = u_weight.shape[1]
    u_pre = jnp.dot(
        normed,
        lax.all_gather(u_weight.astype(jnp.bfloat16), "fs", axis=0, tiled=True),
        preferred_element_type=jnp.float32,
    )
    v_pre = jnp.dot(
        normed,
        lax.all_gather(v_weight.astype(jnp.bfloat16), "fs", axis=0, tiled=True),
        preferred_element_type=jnp.float32,
    )
    u_act = jax.nn.gelu(u_pre * u_scale)
    v_act = jax.nn.gelu(v_pre * v_scale)
    total, squares = lax.psum(
        (jnp.sum(v_act, axis=1, keepdims=True), jnp.sum(v_act * v_act, axis=1, keepdims=True)), "tp"
    )
    branch_width = branch_cols * lax.axis_size("tp")
    centre = total / branch_width
    spread = squares / branch_width - centre * centre
    v_norm = ((v_act - centre) * lax.rsqrt(spread + 1e-06) * v_gain).astype(jnp.bfloat16)
    groups = mix_matrix.shape[0]
    block = mix_matrix.shape[1]
    blocks = v_norm.reshape(rows // block, block, groups, branch_cols // groups)
    mixed = (
        jnp.einsum(
            "gts,bsgd->btgd",
            mix_matrix.astype(jnp.bfloat16),
            blocks,
            preferred_element_type=jnp.float32,
        )
        + mix_bias.T[None, :, :, None]
    )
    gated = (u_act * mixed.reshape(rows, branch_cols)).astype(jnp.bfloat16)
    partial_value = jnp.dot(
        gated,
        lax.all_gather(out_weight.astype(jnp.bfloat16), "fs", axis=1, tiled=True),
        preferred_element_type=jnp.float32,
    )
    mix_out = lax.psum(partial_value.astype(jnp.bfloat16), "tp").astype(jnp.float32) * out_scales
    power = jnp.sum(mix_out * mix_out, axis=1, keepdims=True)
    middle_full = (full_float + rms_norm(mix_out, gain_mix_out, width, power)).astype(jnp.bfloat16)
    middle = lax.dynamic_slice_in_dim(middle_full, lane * part_width, part_width, 1)
    middle_float = middle_full.astype(jnp.float32)
    ffn_in = rms_norm(
        middle_float,
        gain_ffn_in,
        width,
        jnp.sum(middle_float * middle_float, axis=1, keepdims=True),
    ).astype(jnp.bfloat16)
    up_half = up_weight.astype(jnp.bfloat16)
    down_half = down_weight.astype(jnp.bfloat16)
    whole_up = lax.all_gather(up_half, "fs", axis=0, tiled=True)
    raised = jnp.dot(ffn_in, whole_up, preferred_element_type=jnp.float32)
    hidden = jnp.square(jax.nn.relu(raised * up_scale)).astype(jnp.bfloat16)
    whole_down = lax.all_gather(down_half, "fs", axis=1, tiled=True)
    terms = jnp.dot(hidden, whole_down, preferred_element_type=jnp.float32)
    own_down = lax.dynamic_slice_in_dim(down_scales, lane * part_width, part_width, 0)
    ffn_out = (
        lax.psum_scatter(terms.astype(jnp.bfloat16), "tp", scatter_dimension=1, tiled=True).astype(
            jnp.float32
        )
        * own_down
    )
    power_out = lax.psum(jnp.sum(ffn_out * ffn_out, axis=1, keepdims=True), "tp")
    own_gain_out = lax.dynamic_slice_in_dim(gain_ffn_out, lane * part_width, part_width, 0)
    return (middle.astype(jnp.float32) + rms_norm(ffn_out, own_gain_out, width, power_out)).astype(
        jnp.bfloat16
    )


def local_fast(
    resid,
    gain_mix_in,
    u_weight,
    v_weight,
    u_scale,
    v_scale,
    v_gain,
    mix_matrix,
    mix_bias,
    out_weight,
    out_scale,
    gain_mix_out,
    gain_ffn_in,
    up_weight,
    up_scale,
    down_weight,
    down_scale,
    gain_ffn_out,
):
    rows = resid.shape[0]
    part_width = resid.shape[1]
    width = part_width * lax.axis_size("tp")
    lane = lax.axis_index("tp")
    half = jnp.bfloat16
    scale_cols = out_scale.shape[0]
    scales = jnp.concatenate(
        [jnp.broadcast_to(row, (16, scale_cols)) for row in (out_scale, down_scale)]
    )
    shards = [
        v_weight.astype(half),
        u_weight.astype(half),
        out_weight.astype(half),
        scales,
        up_weight.astype(half),
        down_weight.astype(half),
    ]
    whole_v, whole_u, whole_out, whole_scales, whole_up, whole_down, other = gather_all(
        shards, (True, True, False, True, True, False), resid
    )
    whole_scales = whole_scales.reshape(-1, 32, scale_cols)
    out_scales, down_scales = whole_scales[:, 0].reshape(-1), whole_scales[:, 16].reshape(-1)
    swap = [(0, 1), (1, 0)]
    full_rows = jnp.where(
        lane == 0,
        jnp.concatenate([resid, other], axis=1),
        jnp.concatenate([other, resid], axis=1),
    )
    full_float = full_rows.astype(jnp.float32)
    normed = rms_norm(
        full_float, gain_mix_in, width, jnp.sum(full_float * full_float, axis=1, keepdims=True)
    ).astype(jnp.bfloat16)
    branch_cols = u_weight.shape[1]
    u_pre = jnp.dot(
        normed,
        whole_u,
        preferred_element_type=jnp.float32,
    )
    v_pre = jnp.dot(
        normed,
        whole_v,
        preferred_element_type=jnp.float32,
    )
    u_act = jax.nn.gelu(u_pre * u_scale)
    v_act = jax.nn.gelu(v_pre * v_scale)
    total, squares = lax.psum(
        (jnp.sum(v_act, axis=1, keepdims=True), jnp.sum(v_act * v_act, axis=1, keepdims=True)), "tp"
    )
    branch_width = branch_cols * lax.axis_size("tp")
    centre = total / branch_width
    spread = squares / branch_width - centre * centre
    v_norm = ((v_act - centre) * lax.rsqrt(spread + 1e-06) * v_gain).astype(jnp.bfloat16)
    groups = mix_matrix.shape[0]
    block = mix_matrix.shape[1]
    blocks = v_norm.reshape(rows // block, block, groups, branch_cols // groups)
    mixed = (
        jnp.einsum(
            "gts,bsgd->btgd",
            mix_matrix.astype(jnp.bfloat16),
            blocks,
            preferred_element_type=jnp.float32,
        )
        + mix_bias.T[None, :, :, None]
    )
    gated = (u_act * mixed.reshape(rows, branch_cols)).astype(jnp.bfloat16)
    partial_value = jnp.dot(
        gated,
        whole_out,
        preferred_element_type=jnp.float32,
    )
    rounded = partial_value.astype(half)
    mix_out = (
        rounded.astype(jnp.float32) + lax.ppermute(rounded, "tp", swap).astype(jnp.float32)
    ) * out_scales
    power = jnp.sum(mix_out * mix_out, axis=1, keepdims=True)
    middle_full = (full_float + rms_norm(mix_out, gain_mix_out, width, power)).astype(jnp.bfloat16)
    middle = lax.dynamic_slice_in_dim(middle_full, lane * part_width, part_width, 1)
    middle_float = middle_full.astype(jnp.float32)
    ffn_in = rms_norm(
        middle_float,
        gain_ffn_in,
        width,
        jnp.sum(middle_float * middle_float, axis=1, keepdims=True),
    ).astype(jnp.bfloat16)
    raised = jnp.dot(ffn_in, whole_up, preferred_element_type=jnp.float32)
    hidden = jnp.square(jax.nn.relu(raised * up_scale)).astype(jnp.bfloat16)
    terms = jnp.dot(hidden, whole_down, preferred_element_type=jnp.float32)
    own_down = lax.dynamic_slice_in_dim(down_scales, lane * part_width, part_width, 0)
    terms = terms.astype(half)
    kept = lax.dynamic_slice_in_dim(terms, lane * part_width, part_width, 1)
    sent = lax.dynamic_slice_in_dim(terms, (1 - lane) * part_width, part_width, 1)
    ffn_out = (
        kept.astype(jnp.float32) + lax.ppermute(sent, "tp", swap).astype(jnp.float32)
    ) * own_down
    power_out = lax.psum(jnp.sum(ffn_out * ffn_out, axis=1, keepdims=True), "tp")
    own_gain_out = lax.dynamic_slice_in_dim(gain_ffn_out, lane * part_width, part_width, 0)
    return (middle.astype(jnp.float32) + rms_norm(ffn_out, own_gain_out, width, power_out)).astype(
        jnp.bfloat16
    )


def solution(mesh):
    in_specs = (
        P(("rep", "fs"), "tp"),
        P(),
        P("fs", "tp"),
        P("fs", "tp"),
        P("tp"),
        P("tp"),
        P("tp"),
        P("tp", None, None),
        P("tp", None),
        P("tp", "fs"),
        P("fs"),
        P(),
        P(),
        P("fs", "tp"),
        P("tp"),
        P("tp", "fs"),
        P("fs"),
        P(),
    )
    out_specs = P(("rep", "fs"), "tp")
    sizes = mesh.shape

    def whole(*args):
        columns = args[9].shape[1] // sizes["fs"]
        depth = args[2].shape[0] // sizes["fs"]
        paired = sizes["rep"] == 2 and sizes["tp"] == 2 and sizes["fs"] % 2 == 0
        fast = paired and columns % 128 == 0 and depth % 128 == 0
        return mapped(local_fast if fast else local)(*args)

    def mapped(body):
        return jax.shard_map(
            body, mesh=mesh, in_specs=in_specs, out_specs=out_specs, check_vma=False
        )

    return whole
```

```python
import functools

import jax
import jax.numpy as jnp
from jax import lax
from jax.experimental import pallas as pl
from jax.experimental.pallas import tpu as pltpu
from jax.sharding import PartitionSpec as P


def gather_kernel(by_rows, parts, n_out, n_in, *refs):
    count = len(by_rows)
    srcs, resid = refs[:count], refs[count]
    dsts, other = refs[count + 1 : 2 * count + 1], refs[2 * count + 1]
    z_send, z_recv, y_send, y_recv, x_send, x_recv, t_send, t_recv, own_sem = refs[2 * count + 2 :]
    member = lax.axis_index("fs")
    rep = lax.axis_index("rep")
    tp = lax.axis_index("tp")
    outer, inner = member // n_in, member % n_in
    peer_in = 1 - inner
    has_left, has_right = outer > 0, outer < n_out - 1
    left, right = {"fs": member - n_in}, {"fs": member + n_in}
    across, twin, mate = {"fs": outer * n_in + peer_in}, {"rep": 1 - rep}, {"tp": 1 - tp}

    def greet(device):
        pl.semaphore_signal(barrier, inc=1, device_id=device, device_id_type=pl.DeviceIdType.MESH)

    barrier = pltpu.get_barrier_semaphore()
    for step in (1, n_out - 1):
        greet({"fs": lax.rem(outer + step, n_out) * n_in + inner})
    for device in (across, twin, mate):
        greet(device)
    pl.semaphore_wait(barrier, 5)

    def slot(part, index, first=0, length=4):
        w, low, size = parts[part]
        rows, cols = srcs[w].shape
        base, size = low + first * (size // 4), length * (size // 4)
        if by_rows[w]:
            return dsts[w].at[pl.ds(pl.multiple_of(index * rows + base, 8), size), :]
        return dsts[w].at[
            pl.ds(pl.multiple_of(base, 8), size), pl.ds(pl.multiple_of(index * cols, 128), cols)
        ]

    def remote(ref, send, recv, device):
        return pltpu.make_async_remote_copy(
            src_ref=ref,
            dst_ref=ref,
            send_sem=send,
            recv_sem=recv,
            device_id=device,
            device_id_type=pl.DeviceIdType.MESH,
        )

    swap = pltpu.make_async_remote_copy(
        src_ref=resid,
        dst_ref=other,
        send_sem=t_send,
        recv_sem=t_recv,
        device_id=mate,
        device_id_type=pl.DeviceIdType.MESH,
    )
    own = []
    for w in range(count):
        rows, cols = srcs[w].shape
        if by_rows[w]:
            place = dsts[w].at[pl.ds(pl.multiple_of(member * rows, 8), rows), :]
        else:
            place = dsts[w].at[:, pl.ds(pl.multiple_of(member * cols, 128), cols)]
        own.append(pltpu.make_async_copy(srcs[w], place, own_sem.at[w]))
        own[w].start()

    def column(index, line):
        return index * n_in + line

    def z_copy(part, way, d, piece):
        ahead = 1 if way == 0 else -1
        index = column(outer - ahead * d, inner)
        ref = slot(part, index, 2 * rep, 2) if piece == 0 else slot(part, index, 3 * (1 - rep), 1)
        return remote(
            ref,
            z_send.at[part, way, d, piece],
            z_recv.at[part, way, d, piece],
            right if way == 0 else left,
        )

    def valid(way, d):
        return outer >= d if way == 0 else outer + d <= n_out - 1

    def onward(way):
        return has_right if way == 0 else has_left

    def source_of(way, d):
        return outer - d if way == 0 else outer + d

    def y_copy(part, way, d):
        ref = slot(part, column(source_of(way, d), inner), 2 * rep, 2)
        return remote(ref, y_send.at[part, way, d], y_recv.at[part, way, d], across)

    def y_own(part):
        ref = slot(part, member)
        return remote(ref, y_send.at[part, 0, 0], y_recv.at[part, 0, 0], across)

    def x_copy(part, way, d, piece):
        if piece == 0:
            ref = slot(part, column(source_of(way, d), inner), 1 + rep, 1)
        else:
            ref = slot(part, column(source_of(way, d), peer_in), 2 * rep, 2)
        return remote(ref, x_send.at[part, way, d, piece], x_recv.at[part, way, d, piece], twin)

    def landed(part, way, d, piece):
        index = column(source_of(way, d), inner)
        ref = slot(part, index, 2 * rep, 2) if piece == 0 else slot(part, index, 3 * (1 - rep), 1)
        remote(
            ref,
            z_send.at[part, way, d - 1, piece],
            z_recv.at[part, way, d - 1, piece],
            left if way == 0 else right,
        ).wait_recv()

    for w in range(count):
        own[w].wait()
        for part, (held, _, _) in enumerate(parts):
            if held == w:
                for way in range(2):

                    @pl.when(onward(way))
                    def _():
                        z_copy(part, way, 0, 0).start()
                        z_copy(part, way, 0, 1).start()

                y_own(part).start()
        if w == 0:
            swap.start()

    def first_stage(part, way, d):
        @pl.when(valid(way, d))
        def _():
            for piece in range(2):
                landed(part, way, d, piece)
                if d < n_out - 1:
                    pl.when(onward(way))(lambda: z_copy(part, way, d, piece).start())
                if piece == 0:
                    y_copy(part, way, d).start()
                    x_copy(part, way, d, 0).start()

    def second_stage(part, way, d):
        @pl.when(valid(way, d))
        def _():
            y_copy(part, way, d).wait_recv()
            x_copy(part, way, d, 1).start()

    order = [
        (part, way, d) for part in range(len(parts)) for d in range(1, n_out) for way in range(2)
    ]
    lag = 4
    for step in range(len(order) + lag):
        if step < len(order):
            first_stage(*order[step])
        if step >= lag:
            second_stage(*order[step - lag])
    for part, way, d in order:

        @pl.when(valid(way, d))
        def _():
            for piece in range(2):
                x_copy(part, way, d, piece).wait()
                if d < n_out - 1:
                    pl.when(onward(way))(lambda: z_copy(part, way, d, piece).wait_send())
            y_copy(part, way, d).wait_send()

    for part in range(len(parts)):
        y_own(part).wait()
        for way in range(2):

            @pl.when(onward(way))
            def _():
                z_copy(part, way, 0, 0).wait_send()
                z_copy(part, way, 0, 1).wait_send()

    swap.wait()


def gather_all(shards, by_rows, resid):
    members = lax.axis_size("fs")
    n_in = 2
    n_out = members // n_in
    count = len(shards)
    shapes = []
    for shard, rowwise in zip(shards, by_rows):
        rows, cols = shard.shape
        full = (rows * members, cols) if rowwise else (rows, cols * members)
        shapes.append(jax.ShapeDtypeStruct(full, shard.dtype))
    shapes.append(jax.ShapeDtypeStruct(resid.shape, resid.dtype))
    parts = []
    for w, shard in enumerate(shards):
        rows = shard.shape[0]
        pieces = 2 if w >= 4 else 1
        parts += [(w, piece * (rows // pieces), rows // pieces) for piece in range(pieces)]
    many = len(parts)
    pairs = [(many, 2, n_out, 2)] * 2 + [(many, 2, n_out)] * 2 + [(many, 2, n_out, 2)] * 2
    return pl.pallas_call(
        functools.partial(gather_kernel, by_rows, tuple(parts), n_out, n_in),
        out_shape=shapes,
        in_specs=[pl.BlockSpec(memory_space=pltpu.VMEM)] * (count + 1),
        out_specs=[pl.BlockSpec(memory_space=pl.ANY)] * (count + 1),
        scratch_shapes=[pltpu.SemaphoreType.DMA(pair) for pair in pairs]
        + [pltpu.SemaphoreType.DMA, pltpu.SemaphoreType.DMA, pltpu.SemaphoreType.DMA((count,))],
        compiler_params=pltpu.CompilerParams(
            collective_id=0, has_side_effects=True, vmem_limit_bytes=32 * 1024 * 1024
        ),
    )(*shards, resid)


def rms_norm(values, gain, width, power_sum):
    return values * lax.rsqrt(power_sum / width + 1e-06) * gain


def local(
    resid,
    gain_mix_in,
    u_weight,
    v_weight,
    u_scale,
    v_scale,
    v_gain,
    mix_matrix,
    mix_bias,
    out_weight,
    out_scale,
    gain_mix_out,
    gain_ffn_in,
    up_weight,
    up_scale,
    down_weight,
    down_scale,
    gain_ffn_out,
):
    rows = resid.shape[0]
    part_width = resid.shape[1]
    width = part_width * lax.axis_size("tp")
    lane = lax.axis_index("tp")
    full_rows = lax.all_gather(resid, "tp", axis=1, tiled=True)
    out_scales, down_scales = (
        lax.all_gather(out_scale, "fs", axis=0, tiled=True),
        lax.all_gather(down_scale, "fs", axis=0, tiled=True),
    )
    full_float = full_rows.astype(jnp.float32)
    normed = rms_norm(
        full_float, gain_mix_in, width, jnp.sum(full_float * full_float, axis=1, keepdims=True)
    ).astype(jnp.bfloat16)
    branch_cols = u_weight.shape[1]
    u_pre = jnp.dot(
        normed,
        lax.all_gather(u_weight.astype(jnp.bfloat16), "fs", axis=0, tiled=True),
        preferred_element_type=jnp.float32,
    )
    v_pre = jnp.dot(
        normed,
        lax.all_gather(v_weight.astype(jnp.bfloat16), "fs", axis=0, tiled=True),
        preferred_element_type=jnp.float32,
    )
    u_act = jax.nn.gelu(u_pre * u_scale)
    v_act = jax.nn.gelu(v_pre * v_scale)
    total, squares = lax.psum(
        (jnp.sum(v_act, axis=1, keepdims=True), jnp.sum(v_act * v_act, axis=1, keepdims=True)), "tp"
    )
    branch_width = branch_cols * lax.axis_size("tp")
    centre = total / branch_width
    spread = squares / branch_width - centre * centre
    v_norm = ((v_act - centre) * lax.rsqrt(spread + 1e-06) * v_gain).astype(jnp.bfloat16)
    groups = mix_matrix.shape[0]
    block = mix_matrix.shape[1]
    blocks = v_norm.reshape(rows // block, block, groups, branch_cols // groups)
    mixed = (
        jnp.einsum(
            "gts,bsgd->btgd",
            mix_matrix.astype(jnp.bfloat16),
            blocks,
            preferred_element_type=jnp.float32,
        )
        + mix_bias.T[None, :, :, None]
    )
    gated = (u_act * mixed.reshape(rows, branch_cols)).astype(jnp.bfloat16)
    partial_value = jnp.dot(
        gated,
        lax.all_gather(out_weight.astype(jnp.bfloat16), "fs", axis=1, tiled=True),
        preferred_element_type=jnp.float32,
    )
    mix_out = lax.psum(partial_value.astype(jnp.bfloat16), "tp").astype(jnp.float32) * out_scales
    power = jnp.sum(mix_out * mix_out, axis=1, keepdims=True)
    middle_full = (full_float + rms_norm(mix_out, gain_mix_out, width, power)).astype(jnp.bfloat16)
    middle = lax.dynamic_slice_in_dim(middle_full, lane * part_width, part_width, 1)
    middle_float = middle_full.astype(jnp.float32)
    ffn_in = rms_norm(
        middle_float,
        gain_ffn_in,
        width,
        jnp.sum(middle_float * middle_float, axis=1, keepdims=True),
    ).astype(jnp.bfloat16)
    up_half = up_weight.astype(jnp.bfloat16)
    down_half = down_weight.astype(jnp.bfloat16)
    whole_up = lax.all_gather(up_half, "fs", axis=0, tiled=True)
    raised = jnp.dot(ffn_in, whole_up, preferred_element_type=jnp.float32)
    hidden = jnp.square(jax.nn.relu(raised * up_scale)).astype(jnp.bfloat16)
    whole_down = lax.all_gather(down_half, "fs", axis=1, tiled=True)
    terms = jnp.dot(hidden, whole_down, preferred_element_type=jnp.float32)
    own_down = lax.dynamic_slice_in_dim(down_scales, lane * part_width, part_width, 0)
    ffn_out = (
        lax.psum_scatter(terms.astype(jnp.bfloat16), "tp", scatter_dimension=1, tiled=True).astype(
            jnp.float32
        )
        * own_down
    )
    power_out = lax.psum(jnp.sum(ffn_out * ffn_out, axis=1, keepdims=True), "tp")
    own_gain_out = lax.dynamic_slice_in_dim(gain_ffn_out, lane * part_width, part_width, 0)
    return (middle.astype(jnp.float32) + rms_norm(ffn_out, own_gain_out, width, power_out)).astype(
        jnp.bfloat16
    )


def local_fast(
    resid,
    gain_mix_in,
    u_weight,
    v_weight,
    u_scale,
    v_scale,
    v_gain,
    mix_matrix,
    mix_bias,
    out_weight,
    out_scale,
    gain_mix_out,
    gain_ffn_in,
    up_weight,
    up_scale,
    down_weight,
    down_scale,
    gain_ffn_out,
):
    rows = resid.shape[0]
    part_width = resid.shape[1]
    width = part_width * lax.axis_size("tp")
    lane = lax.axis_index("tp")
    half = jnp.bfloat16
    scale_cols = out_scale.shape[0]
    scales = jnp.concatenate(
        [jnp.broadcast_to(row, (16, scale_cols)) for row in (out_scale, down_scale)]
    )
    shards = [
        v_weight.astype(half),
        u_weight.astype(half),
        out_weight.astype(half),
        scales,
        up_weight.astype(half),
    ]
    whole_down = lax.all_gather(down_weight.astype(half), "fs", axis=1, tiled=True)
    whole_v, whole_u, whole_out, whole_scales, whole_up, other = gather_all(
        shards, (True, True, False, True, True), resid
    )
    whole_scales = whole_scales.reshape(-1, 32, scale_cols)
    out_scales, down_scales = whole_scales[:, 0].reshape(-1), whole_scales[:, 16].reshape(-1)
    swap = [(0, 1), (1, 0)]
    full_rows = jnp.where(
        lane == 0,
        jnp.concatenate([resid, other], axis=1),
        jnp.concatenate([other, resid], axis=1),
    )
    full_float = full_rows.astype(jnp.float32)
    normed = rms_norm(
        full_float, gain_mix_in, width, jnp.sum(full_float * full_float, axis=1, keepdims=True)
    ).astype(jnp.bfloat16)
    branch_cols = u_weight.shape[1]
    u_pre = jnp.dot(
        normed,
        whole_u,
        preferred_element_type=jnp.float32,
    )
    v_pre = jnp.dot(
        normed,
        whole_v,
        preferred_element_type=jnp.float32,
    )
    u_act = jax.nn.gelu(u_pre * u_scale)
    v_act = jax.nn.gelu(v_pre * v_scale)
    total, squares = lax.psum(
        (jnp.sum(v_act, axis=1, keepdims=True), jnp.sum(v_act * v_act, axis=1, keepdims=True)), "tp"
    )
    branch_width = branch_cols * lax.axis_size("tp")
    centre = total / branch_width
    spread = squares / branch_width - centre * centre
    v_norm = ((v_act - centre) * lax.rsqrt(spread + 1e-06) * v_gain).astype(jnp.bfloat16)
    groups = mix_matrix.shape[0]
    block = mix_matrix.shape[1]
    blocks = v_norm.reshape(rows // block, block, groups, branch_cols // groups)
    mixed = (
        jnp.einsum(
            "gts,bsgd->btgd",
            mix_matrix.astype(jnp.bfloat16),
            blocks,
            preferred_element_type=jnp.float32,
        )
        + mix_bias.T[None, :, :, None]
    )
    gated = (u_act * mixed.reshape(rows, branch_cols)).astype(jnp.bfloat16)
    partial_value = jnp.dot(
        gated,
        whole_out,
        preferred_element_type=jnp.float32,
    )
    rounded = partial_value.astype(half)
    mix_out = (
        rounded.astype(jnp.float32) + lax.ppermute(rounded, "tp", swap).astype(jnp.float32)
    ) * out_scales
    power = jnp.sum(mix_out * mix_out, axis=1, keepdims=True)
    middle_full = (full_float + rms_norm(mix_out, gain_mix_out, width, power)).astype(jnp.bfloat16)
    middle = lax.dynamic_slice_in_dim(middle_full, lane * part_width, part_width, 1)
    middle_float = middle_full.astype(jnp.float32)
    ffn_in = rms_norm(
        middle_float,
        gain_ffn_in,
        width,
        jnp.sum(middle_float * middle_float, axis=1, keepdims=True),
    ).astype(jnp.bfloat16)
    raised = jnp.dot(ffn_in, whole_up, preferred_element_type=jnp.float32)
    hidden = jnp.square(jax.nn.relu(raised * up_scale)).astype(jnp.bfloat16)
    terms = jnp.dot(hidden, whole_down, preferred_element_type=jnp.float32)
    own_down = lax.dynamic_slice_in_dim(down_scales, lane * part_width, part_width, 0)
    terms = terms.astype(half)
    kept = lax.dynamic_slice_in_dim(terms, lane * part_width, part_width, 1)
    sent = lax.dynamic_slice_in_dim(terms, (1 - lane) * part_width, part_width, 1)
    ffn_out = (
        kept.astype(jnp.float32) + lax.ppermute(sent, "tp", swap).astype(jnp.float32)
    ) * own_down
    power_out = lax.psum(jnp.sum(ffn_out * ffn_out, axis=1, keepdims=True), "tp")
    own_gain_out = lax.dynamic_slice_in_dim(gain_ffn_out, lane * part_width, part_width, 0)
    return (middle.astype(jnp.float32) + rms_norm(ffn_out, own_gain_out, width, power_out)).astype(
        jnp.bfloat16
    )


def solution(mesh):
    in_specs = (
        P(("rep", "fs"), "tp"),
        P(),
        P("fs", "tp"),
        P("fs", "tp"),
        P("tp"),
        P("tp"),
        P("tp"),
        P("tp", None, None),
        P("tp", None),
        P("tp", "fs"),
        P("fs"),
        P(),
        P(),
        P("fs", "tp"),
        P("tp"),
        P("tp", "fs"),
        P("fs"),
        P(),
    )
    out_specs = P(("rep", "fs"), "tp")
    sizes = mesh.shape

    def whole(*args):
        columns = args[9].shape[1] // sizes["fs"]
        depth = args[2].shape[0] // sizes["fs"]
        paired = sizes["rep"] == 2 and sizes["tp"] == 2 and sizes["fs"] % 2 == 0
        fast = paired and columns % 128 == 0 and depth % 128 == 0
        return mapped(local_fast if fast else local)(*args)

    def mapped(body):
        return jax.shard_map(
            body, mesh=mesh, in_specs=in_specs, out_specs=out_specs, check_vma=False
        )

    return whole
```
